32 devices in a mesh: sp: 8 (over z, core), tp: 4 (over y, x).
Axes of the slice: x: 2, y: 2, z: 4, core: 2. Of those that a mesh axis runs over, the one named last changes fastest.
Arguments:
- queries: bfloat16 [2048, 2048], P('sp', 'tp'), may hold values from -6 to 6
- keys: bfloat16 [2048, 1024], P('sp', 'tp'), may hold values from -6 to 6
- values: bfloat16 [2048, 1024], P('sp', 'tp'), may hold values from -6 to 6
- sink_logit: float32 [32], P('tp'), may hold values from -1 to 6
- out_weight: bfloat16 [2048, 2048], P(None, 'tp'), may hold values from -0.125 to 0.125
- residual: bfloat16 [2048, 2048], P(('sp', 'tp')), may hold values from -1.796875 to 1.796875
- norm_gain: float32 [2048], replicated, may hold values from 0.1 to 1.9
- routes: int32 [2048, 2], P(('sp', 'tp')), may hold values from 0 to 7, all different within a row; in each aligned block of 64 rows (0 to 63, 64 to 127, ...) at most 32 rows name the same one
- route_weights: float32 [2048, 2], P(('sp', 'tp')), may hold values from 0.2 to 1
- gate_weight: bfloat16 [8, 2048, 5120], P('sp', None, 'tp'), may hold values from -0.125 to 0.125
- up_weight: bfloat16 [8, 2048, 5120], P('sp', None, 'tp'), may hold values from -0.125 to 0.125
- down_weight: bfloat16 [8, 5120, 2048], P('sp', 'tp'), may hold values from -0.078125 to 0.078125
Outputs:
- mixed: bfloat16 [2048, 2048], P(('sp', 'tp'))
The draws below stay inside these ranges and needn't reach their ends.
Inputs may be any that keep to these rules, and one draw needn't show every extreme that they name: `routes`: each row names two different experts. Among the rows of one device no expert is named more than 32 times, and in every draw some expert is named exactly 32 times by the rows of some device.
All inputs are finite; a program needn't handle non-finite values.
Results may differ from the reference program's by a relative error of at most 0.018.
Values may be sent and summed in bfloat16 or wider, within the bound.
A program may use at most 64 MiB of HBM per device.

```python
import math
import jax
import jax.numpy as jnp
import numpy as np
from jax import lax

D = 2048
FF = 5120
HEADS = 32
KV_HEADS = 16
HEAD = 64
WINDOW = 128
TOK_DEV = 64
TOKENS = 2048
EXPERTS = 8
CAP = 32
N_SP = 8
N_TP = 4


def draw_queries(key, part):
    own_key = jax.random.fold_in(key, 17)
    drawn = jnp.clip(jax.random.normal(own_key, (TOKENS, HEADS * HEAD), jnp.float32), -6.0, 6.0)
    return drawn.astype(jnp.bfloat16)


def draw_keys(key, part):
    own_key = jax.random.fold_in(key, 29)
    drawn = jnp.clip(jax.random.normal(own_key, (TOKENS, KV_HEADS * HEAD), jnp.float32), -6.0, 6.0)
    return drawn.astype(jnp.bfloat16)


def shard_levels(stream_key, dims, cuts, smallest, top_value):
    level = 1.0
    for position, shards_of in cuts:
        steps = jax.random.uniform(jax.random.fold_in(jax.random.fold_in(stream_key, 6), position), (shards_of,), jnp.float32, smallest / len(cuts), top_value / len(cuts))
        level = level * jnp.repeat(jnp.exp(steps), dims[position] // shards_of).reshape((-1,) + (1,) * (len(dims) - 1 - position))
    return level


def deal_out(rng, own, number, rows, amount, top, limit, lean):
    order = jax.random.permutation(rng, amount)
    packed, ordinary = portions_of(amount, rows * top, limit, lean, True), portions_of(amount, rows * top, limit, lean, False)
    places = jnp.arange(amount)

    def named(tallies, rotation):
        used = int((tallies > 0).sum())
        fixed = max(1, used // 4)
        moved = fixed + (places - fixed + rotation * (used - fixed)) % max(1, amount - fixed)
        return jnp.zeros((amount,), jnp.int32).at[order[jnp.where(places < fixed, places, moved)]].set(jnp.asarray(tallies, jnp.int32))

    tallies = jnp.where(number % 4 == 0, named(packed, number // 4), named(ordinary, number - number // 4 - 1))
    mixed = jax.random.permutation(jax.random.fold_in(own, 3), amount)
    donor, taker = mixed[0:amount // 2 * 2:2], mixed[1:amount // 2 * 2:2]
    slack = jnp.minimum(tallies[donor] - 1, limit - tallies[taker]) // 2
    slack = jnp.where((donor == order[0]) | (taker == order[0]) | (tallies[taker] == 0), 0, jnp.maximum(slack, 0))
    moved = jax.random.randint(jax.random.fold_in(own, 4), (amount // 2,), 0, 1 << 20) % (slack + 1)
    tallies = tallies.at[donor].add(-moved).at[taker].add(moved)
    members = jnp.searchsorted(jnp.cumsum(tallies), jnp.arange(rows * top), side="right").astype(jnp.int32)
    listing = members.reshape(top, rows).T
    listing = listing[jax.random.permutation(jax.random.fold_in(own, 1), rows)]
    rotation = jax.random.randint(jax.random.fold_in(own, 2), (rows, 1), 0, top)
    return jnp.take_along_axis(listing, (jnp.arange(top)[None, :] + rotation) % top, axis=1)


def portions_of(amount, total, most, lean, full):
    loads = [(1 << 20) // math.isqrt(rank ** lean) + 1 for rank in range(1, amount + 1)]
    largest = most if full else min(most, max(-(-total // amount), total * loads[0] // sum(loads)))
    least = 1 if total - largest >= amount - 1 else 0
    counts, surplus = [largest] + [least] * (amount - 1), total - largest - least * (amount - 1)
    while surplus > 0:
        movable = [i for i in range(1, amount) if counts[i] < largest] or [i for i in range(1, amount) if counts[i] < most]
        pool, remaining = sum([loads[i] for i in movable]), surplus
        for i in movable:
            more = min(most - counts[i], max(1, remaining * loads[i] // pool), surplus)
            counts[i] = counts[i] + more
            surplus = surplus - more
    return np.array(counts)


def scatter_about(stream_key, extent, width, bound, shards=(), held_as=jnp.bfloat16):
    array = width * jax.random.normal(stream_key, extent, jnp.float32)
    if shards:
        array = array * shard_levels(stream_key, extent, shards, -0.22, 0.18)
    return jnp.clip(array, -bound, bound).astype(held_as)


def setup_inputs(seed: int = 0) -> dict:
    key_of = jax.random.split(jax.random.key(seed), 13)
    queries = draw_queries(jax.random.fold_in(key_of[12], 71), 0)
    keys = draw_keys(jax.random.fold_in(key_of[12], 71), 0)
    values = scatter_about(key_of[2], (TOKENS, KV_HEADS * HEAD), 1.0, 6.0, ((0, 8), (1, 4)))
    sink_logit = jnp.clip(-1.0 + 7.0 * jax.random.uniform(key_of[3], (HEADS,), jnp.float32) ** shard_levels(key_of[3], (HEADS,), ((0, 4),), -0.2, 0.2), -1.0, 6.0)
    out_weight = scatter_about(key_of[4], (HEADS * HEAD, D), (HEADS * HEAD) ** -0.5, 0.125, ((1, 4),))
    residual = scatter_about(key_of[5], (TOKENS, D), 0.3, 1.796875, ((0, 32),))
    norm_gain = jnp.clip(1.0 + 0.18 * jax.random.normal(key_of[6], (D,), jnp.float32), 0.1, 1.9)
    routes_keys = jax.random.split(jax.random.fold_in(key_of[7], 1), TOKENS // TOK_DEV)
    routes_turns = jax.random.permutation(jax.random.fold_in(key_of[7], 3), TOKENS // TOK_DEV)
    routes = jax.vmap(lambda own, number: deal_out(jax.random.fold_in(key_of[7], 2), own, number, TOK_DEV, EXPERTS, 2, CAP, 1))(routes_keys, routes_turns).reshape((TOKENS, 2))
    route_weights = jnp.clip(0.2 + 0.8 * jax.random.uniform(key_of[8], (TOKENS, 2), jnp.float32) ** shard_levels(key_of[8], (TOKENS, 2), ((0, 32),), -0.2, 0.2), 0.2, 1.0)
    gate_weight = scatter_about(key_of[9], (EXPERTS, D, FF), D ** -0.5, 0.125, ((0, 8), (2, 4)))
    up_weight = scatter_about(key_of[10], (EXPERTS, D, FF), D ** -0.5, 0.125, ((0, 8), (2, 4)))
    down_weight = scatter_about(key_of[11], (EXPERTS, FF, D), FF ** -0.5, 0.078125, ((0, 8), (1, 4)))
    return {"queries": queries, "keys": keys, "values": values, "sink_logit": sink_logit, "out_weight": out_weight, "residual": residual, "norm_gain": norm_gain, "routes": routes, "route_weights": route_weights, "gate_weight": gate_weight, "up_weight": up_weight, "down_weight": down_weight}


EPS = 1e-06
NEGATIVE = -1e+30

def make_band(tensor):
    length = tensor.shape[0]
    blocks = length // WINDOW
    padded = jnp.pad(tensor, ((WINDOW, WINDOW), (0, 0)))
    pieces = [padded[offset * WINDOW:offset * WINDOW + length].reshape(blocks, WINDOW, -1) for offset in range(3)]
    return jnp.concatenate(pieces, axis=1)

def attend(queries, keys, values, sink_logit):
    tokens = queries.shape[0]
    blocks = tokens // WINDOW
    repeat = HEADS // KV_HEADS
    scale = HEAD ** (-0.5)
    near = jnp.abs(jnp.arange(WINDOW)[:, None] + WINDOW - jnp.arange(3 * WINDOW)[None, :]) <= WINDOW
    key_pos = (jnp.arange(blocks)[:, None] - 1) * WINDOW + jnp.arange(3 * WINDOW)[None, :]
    inside = (key_pos >= 0) & (key_pos < tokens)
    valid = near[None, None, :, :] & inside[:, None, None, :]
    query_groups = queries.reshape(tokens, KV_HEADS, repeat, HEAD).transpose(1, 0, 2, 3)
    key_groups = keys.reshape(tokens, KV_HEADS, HEAD).transpose(1, 0, 2)
    value_groups = values.reshape(tokens, KV_HEADS, HEAD).transpose(1, 0, 2)
    sink_groups = sink_logit.reshape(KV_HEADS, repeat)

    def one_group(inputs):
        query_rows, key_rows, value_rows, sinks = inputs
        query_blocks = query_rows.reshape(blocks, WINDOW, repeat, HEAD).astype(jnp.float32)
        key_band = make_band(key_rows).astype(jnp.float32)
        value_band = make_band(value_rows).astype(jnp.float32)
        scores = jnp.einsum('nqrd,nkd->nrqk', query_blocks, key_band) * scale
        sink = sinks.astype(jnp.float32)[None, :, None, None]
        masked = jnp.where(valid, scores, NEGATIVE)
        top = jnp.maximum(lax.optimization_barrier(jnp.max(masked, axis=-1, keepdims=True)), sink)
        probs = jnp.exp(masked - top)
        denom = lax.optimization_barrier(jnp.sum(probs, axis=-1, keepdims=True)) + jnp.exp(sink - top)
        weights = (probs / denom).astype(jnp.bfloat16)
        output = jnp.einsum('nrqk,nkd->nqrd', weights.astype(jnp.float32), value_band)
        return output.astype(jnp.bfloat16).reshape(tokens, repeat * HEAD)
    outputs = lax.map(one_group, (query_groups, key_groups, value_groups, sink_groups))
    return outputs.transpose(1, 0, 2).reshape(tokens, HEADS * HEAD)

def one_expert(inputs):
    rows, gate_matrix, up_matrix, down_matrix = inputs
    gate = jnp.dot(rows, gate_matrix, preferred_element_type=jnp.float32)
    upward = jnp.dot(rows, up_matrix, preferred_element_type=jnp.float32)
    hidden = (jax.nn.silu(gate) * upward).astype(jnp.bfloat16)
    block_width = FF // N_TP
    shares = jnp.einsum('rjf,jfd->jrd', hidden.reshape(-1, N_TP, block_width).astype(jnp.float32), down_matrix.reshape(N_TP, block_width, D).astype(jnp.float32))
    return lax.optimization_barrier(jnp.sum(shares.astype(jnp.bfloat16).astype(jnp.float32), axis=0)).astype(jnp.bfloat16)

def reference(queries, keys, values, sink_logit, out_weight, residual, norm_gain, routes, route_weights, gate_weight, up_weight, down_weight):
    attention = attend(queries, keys, values, sink_logit)
    projected = jnp.dot(attention, out_weight, preferred_element_type=jnp.float32).astype(jnp.bfloat16)
    hidden_state = residual.astype(jnp.float32) + projected.astype(jnp.float32)
    inverse = lax.rsqrt(lax.optimization_barrier(jnp.mean(hidden_state * hidden_state, axis=-1, keepdims=True)) + EPS)
    normed = (hidden_state * inverse * norm_gain).astype(jnp.bfloat16)
    devices = N_SP * N_TP
    expert_ids = routes.reshape(devices, 2 * TOK_DEV).astype(jnp.int32)
    onehot = (expert_ids[..., None] == jnp.arange(EXPERTS, dtype=jnp.int32)).astype(jnp.int32)
    earlier = jnp.cumsum(onehot, axis=1) - onehot
    rank = lax.optimization_barrier(jnp.sum(earlier * onehot, axis=-1))
    slots = (jnp.arange(devices, dtype=jnp.int32)[:, None] * CAP + rank).reshape(-1).astype(jnp.int32)
    flat_ids = expert_ids.reshape(-1)
    pair_rows = jnp.repeat(normed, 2, axis=0)
    buffer = jnp.zeros((EXPERTS, devices * CAP, D), jnp.bfloat16).at[flat_ids, slots].set(pair_rows)
    expert_out = lax.map(one_expert, (buffer, gate_weight, up_weight, down_weight))
    picked = expert_out[flat_ids, slots].reshape(TOKENS, 2, D).astype(jnp.float32)
    mixture = lax.optimization_barrier(jnp.sum(route_weights[..., None] * picked, axis=1))
    return (hidden_state + mixture).astype(jnp.bfloat16)
```

```python
import functools

import jax
import jax.numpy as jnp
from jax import lax
from jax.experimental import pallas as pl
from jax.experimental.pallas import tpu as pltpu
from jax.sharding import PartitionSpec as P

HEADS = 32
KV_HEADS = 16
HEAD = 64
WINDOW = 128


EPS = 1e-06
NEGATIVE = -1e30
MESH = pl.DeviceIdType.MESH


def plane():
    t = lax.axis_index("tp")
    tx = t + 1 - 2 * lax.rem(t, 2)
    ty = lax.rem(t + 2, 4)
    return t, tx, ty, 3 - t


def greet(devices):
    barrier = pltpu.get_barrier_semaphore()
    for device in devices:
        pl.semaphore_signal(barrier, inc=1, device_id=device, device_id_type=MESH)
    pl.semaphore_wait(barrier, len(devices))


def remote(src, dst, send, recv, device):
    return pltpu.make_async_remote_copy(
        src_ref=src,
        dst_ref=dst,
        send_sem=send,
        recv_sem=recv,
        device_id=device,
        device_id_type=MESH,
    )


def dispatch_kernel(n, send_ref, out_ref, zs, zr, xs, xr, ys, yr, xhs, xhr, yhs, yhr):
    s = lax.axis_index("sp")
    t, tx, ty, _ = plane()
    half = send_ref.shape[1] // 2
    low, high = pl.ds(0, half), pl.ds(half, half)
    x_dev, y_dev = (s, tx), (s, ty)
    greet([(lax.rem(s + k, n), t) for k in range(1, n)] + [x_dev, y_dev])
    copies = []

    def go(*args):
        copy = remote(*args)
        copy.start()
        copies.append(copy)
        return copy

    incoming = [None]
    full = []

    def stage_a(j):
        source = lax.rem(s - j + n, n)
        if j:
            z_copies[j].wait_recv()
        src = out_ref.at[t, source] if j else send_ref.at[source]
        full.append(
            (
                go(src, out_ref.at[t, source], xs.at[j], xr.at[j], x_dev),
                go(src, out_ref.at[t, source], ys.at[j], yr.at[j], y_dev),
            )
        )

    halves = []

    def stage_b(j):
        source = lax.rem(s - j + n, n)
        full[j][0].wait_recv()
        part = out_ref.at[tx, source, low]
        halves.append(go(part, part, yhs.at[j], yhr.at[j], y_dev))
        full[j][1].wait_recv()
        part = out_ref.at[ty, source, high]
        halves.append(go(part, part, xhs.at[j], xhr.at[j], x_dev))

    z_copies = [None]
    for k in range(1, n):
        target = lax.rem(s + k, n)
        z_copies.append(
            go(send_ref.at[target], out_ref.at[t, s], zs.at[k], zr.at[k], (target, t))
        )
    stage_a(0)
    out_ref[t, s] = send_ref[s]
    for j in range(1, n):
        stage_a(j)
        stage_b(j - 1)
    stage_b(n - 1)
    for copy in halves:
        copy.wait_recv()
    for copy in copies:
        copy.wait_send()


def dispatch(sending):
    n, capacity, width = sending.shape
    sem = pltpu.SemaphoreType.DMA((n,))
    return pl.pallas_call(
        functools.partial(dispatch_kernel, n),
        out_shape=jax.ShapeDtypeStruct((4, n, capacity, width), sending.dtype),
        in_specs=[pl.BlockSpec(memory_space=pltpu.VMEM)],
        out_specs=pl.BlockSpec(memory_space=pltpu.VMEM),
        scratch_shapes=[sem] * 10,
        compiler_params=pltpu.CompilerParams(collective_id=0, has_side_effects=True),
    )(sending)


def return_kernel(
    n, part_ref, out_ref, bx1, by1, bx2, by2, acc, fin,
    x1s, x1r, y1s, y1r, x2s, x2r, y2s, y2r, zls, zlr, zhs, zhr,
):
    s = lax.axis_index("sp")
    t, tx, ty, td = plane()
    half = part_ref.shape[2] // 2
    low, high = pl.ds(0, half), pl.ds(half, half)
    x_dev, y_dev = (s, tx), (s, ty)
    greet([(lax.rem(s + k, n), t) for k in range(1, n)] + [x_dev, y_dev])
    copies = []

    def go(*args):
        copy = remote(*args)
        copy.start()
        copies.append(copy)
        return copy

    def total(a, b):
        return (a.astype(jnp.float32) + b.astype(jnp.float32)).astype(jnp.bfloat16)

    order = list(range(1, n)) + [0]
    first = []
    for j in order:
        owner = lax.rem(s + j, n)
        first.append(
            (
                go(part_ref.at[td, owner, low], bx1.at[j, 1], x1s.at[j, 1], x1r.at[j, 1], x_dev),
                go(part_ref.at[td, owner, high], by1.at[j, 1], y1s.at[j, 1], y1r.at[j, 1], y_dev),
                go(part_ref.at[tx, owner, low], bx1.at[j, 0], x1s.at[j, 0], x1r.at[j, 0], x_dev),
                go(part_ref.at[ty, owner, high], by1.at[j, 0], y1s.at[j, 0], y1r.at[j, 0], y_dev),
            )
        )
    second = []
    back = []

    def middle(i):
        j = order[i]
        owner = lax.rem(s + j, n)
        first[i][0].wait_recv()
        acc[j, 0] = total(part_ref[ty, owner, low], bx1[j, 1])
        to_y = go(acc.at[j, 0], by2.at[j], y2s.at[j], y2r.at[j], y_dev)
        first[i][1].wait_recv()
        acc[j, 1] = total(part_ref[tx, owner, high], by1[j, 1])
        to_x = go(acc.at[j, 1], bx2.at[j], x2s.at[j], x2r.at[j], x_dev)
        second.append((to_y, to_x))

    def last(i):
        j = order[i]
        owner = lax.rem(s + j, n)
        first[i][2].wait_recv()
        second[i][0].wait_recv()
        lower = total(
            part_ref[t, owner, low].astype(jnp.float32) + bx1[j, 0].astype(jnp.float32), by2[j]
        )
        first[i][3].wait_recv()
        second[i][1].wait_recv()
        upper = total(
            part_ref[t, owner, high].astype(jnp.float32) + by1[j, 0].astype(jnp.float32), bx2[j]
        )
        if j:
            fin[j, low] = lower
            back.append(go(fin.at[j, low], out_ref.at[s, low], zls.at[j], zlr.at[j], (owner, t)))
            fin[j, high] = upper
            back.append(go(fin.at[j, high], out_ref.at[s, high], zhs.at[j], zhr.at[j], (owner, t)))
        else:
            out_ref[s, low] = lower
            out_ref[s, high] = upper

    middle(0)
    for i in range(1, n):
        middle(i)
        last(i - 1)
    last(n - 1)
    for copy in back:
        copy.wait_recv()
    for copy in copies:
        copy.wait_send()


def give_back(partial_value):
    _, n, capacity, width = partial_value.shape
    half = capacity // 2
    kind = partial_value.dtype
    one = pltpu.SemaphoreType.DMA((n,))
    two = pltpu.SemaphoreType.DMA((n, 2))
    return pl.pallas_call(
        functools.partial(return_kernel, n),
        out_shape=jax.ShapeDtypeStruct((n, capacity, width), kind),
        in_specs=[pl.BlockSpec(memory_space=pltpu.VMEM)],
        out_specs=pl.BlockSpec(memory_space=pltpu.VMEM),
        scratch_shapes=[
            pltpu.VMEM((n, 2, half, width), kind),
            pltpu.VMEM((n, 2, half, width), kind),
            pltpu.VMEM((n, half, width), kind),
            pltpu.VMEM((n, half, width), kind),
            pltpu.VMEM((n, 2, half, width), kind),
            pltpu.VMEM((n, capacity, width), kind),
            two, two, two, two, one, one, one, one, one, one, one, one,
        ],
        compiler_params=pltpu.CompilerParams(collective_id=1, has_side_effects=True),
    )(partial_value)


def with_halo(block, sides, width):
    for axis, dim in sides:
        count = lax.axis_size(axis)
        forward = [(i, i + 1) for i in range(count - 1)]
        backward = [(target, source) for source, target in forward]
        low = lax.ppermute(
            lax.slice_in_dim(block, block.shape[dim] - width, None, axis=dim), axis, forward
        )
        high = lax.ppermute(lax.slice_in_dim(block, 0, width, axis=dim), axis, backward)
        block = jnp.concatenate([low, block, high], axis=dim)
    return block


def make_band(extended, length):
    blocks = length // WINDOW
    pieces = [
        lax.slice_in_dim(extended, offset * WINDOW, offset * WINDOW + length, axis=0).reshape(
            blocks, WINDOW, -1
        )
        for offset in range(3)
    ]
    return jnp.concatenate(pieces, axis=1)


def attend_local(queries, keys, values, sink_logit):
    length = queries.shape[0]
    groups = keys.shape[1] // HEAD
    repeat = HEADS // KV_HEADS
    blocks = length // WINDOW
    joined = jnp.concatenate([keys, values], axis=1)
    extended = with_halo(joined, (("sp", 0),), WINDOW)
    banded = make_band(extended, length)
    key_band = banded[..., : groups * HEAD].reshape(blocks, 3 * WINDOW, groups, HEAD)
    value_band = banded[..., groups * HEAD :].reshape(blocks, 3 * WINDOW, groups, HEAD)
    query_blocks = queries.reshape(blocks, WINDOW, groups, repeat, HEAD)
    scores = jnp.einsum(
        "nqgrd,nkgd->ngrqk", query_blocks, key_band, preferred_element_type=jnp.float32
    ) * HEAD ** (-0.5)
    near = jnp.abs(jnp.arange(WINDOW)[:, None] + WINDOW - jnp.arange(3 * WINDOW)[None, :]) <= WINDOW
    first_token = lax.axis_index("sp") * length
    key_pos = (
        first_token + (jnp.arange(blocks)[:, None] - 1) * WINDOW + jnp.arange(3 * WINDOW)[None, :]
    )
    inside = (key_pos >= 0) & (key_pos < length * lax.axis_size("sp"))
    valid = near[None, None, None, :, :] & inside[:, None, None, None, :]
    sinks = sink_logit.reshape(1, groups, repeat, 1, 1)
    masked = jnp.where(valid, scores, NEGATIVE)
    top = jnp.maximum(jnp.max(masked, axis=-1, keepdims=True), sinks)
    probs = jnp.exp(masked - top)
    denom = jnp.sum(probs, axis=-1, keepdims=True) + jnp.exp(sinks - top)
    weights = (probs / denom).astype(jnp.bfloat16)
    output = jnp.einsum(
        "ngrqk,nkgd->nqgrd", weights, value_band, preferred_element_type=jnp.float32
    )
    return output.astype(jnp.bfloat16).reshape(length, groups * repeat * HEAD)


def local(
    queries,
    keys,
    values,
    sink_logit,
    out_weight,
    residual,
    norm_gain,
    routes,
    route_weights,
    gate_weight,
    up_weight,
    down_weight,
):
    attention = attend_local(queries, keys, values, sink_logit)
    columns = jnp.dot(
        lax.all_gather(attention, "tp", axis=1, tiled=True),
        out_weight,
        preferred_element_type=jnp.float32,
    )
    projected = lax.all_to_all(
        columns.astype(jnp.bfloat16), "tp", split_axis=0, concat_axis=1, tiled=True
    )
    hidden_state = residual.astype(jnp.float32) + projected.astype(jnp.float32)
    inverse = lax.rsqrt(jnp.mean(hidden_state * hidden_state, axis=-1, keepdims=True) + EPS)
    normed = (hidden_state * inverse * norm_gain).astype(jnp.bfloat16)
    sp_count = lax.axis_size("sp")
    tok_rows = residual.shape[0]
    width = residual.shape[1]
    capacity = max(2, 4 * tok_rows // sp_count)
    slot_total = sp_count * capacity
    expert_ids = routes.reshape(-1)
    onehot = (expert_ids[:, None] == jnp.arange(sp_count, dtype=jnp.int32)[None, :]).astype(
        jnp.int32
    )
    earlier = jnp.cumsum(onehot, axis=0) - onehot
    rank = jnp.sum(earlier * onehot, axis=1)
    slots = expert_ids * capacity + rank
    placing = (slots[:, None] == jnp.arange(slot_total, dtype=jnp.int32)[None, :]).astype(
        jnp.bfloat16
    )
    placing = placing.reshape(tok_rows, 2, slot_total)
    first_place = placing[:, 0]
    second_place = placing[:, 1]
    sending = jnp.einsum(
        "ts,td->sd", first_place + second_place, normed, preferred_element_type=jnp.float32
    )
    sending = sending.astype(jnp.bfloat16).reshape(sp_count, capacity, width)
    in_plane = lax.axis_size("tp") == 4 and capacity % 32 == 0
    if in_plane:
        piece = dispatch(sending)
    else:
        piece = lax.all_gather(
            lax.all_to_all(sending, "sp", split_axis=0, concat_axis=0, tiled=True),
            "tp",
            axis=0,
            tiled=True,
        )
    flat = piece.reshape(-1, piece.shape[-1])
    gate = jnp.dot(flat, gate_weight[0], preferred_element_type=jnp.float32)
    upward = jnp.dot(flat, up_weight[0], preferred_element_type=jnp.float32)
    hidden = (jax.nn.silu(gate) * upward).astype(jnp.bfloat16)
    partial_value = jnp.dot(hidden, down_weight[0], preferred_element_type=jnp.float32)
    partial_value = partial_value.reshape(piece.shape[:-1] + (down_weight.shape[-1],))
    partial_value = partial_value.astype(jnp.bfloat16)
    if in_plane:
        returned = give_back(partial_value)
    else:
        returned = lax.all_to_all(
            lax.psum_scatter(partial_value, "tp", scatter_dimension=0, tiled=True),
            "sp",
            split_axis=0,
            concat_axis=0,
            tiled=True,
        )
    gathered_back = returned.reshape(slot_total, width)
    first_pick = jnp.dot(first_place, gathered_back, preferred_element_type=jnp.float32)
    second_pick = jnp.dot(second_place, gathered_back, preferred_element_type=jnp.float32)
    mixture = route_weights[:, 0:1] * first_pick + route_weights[:, 1:2] * second_pick
    return (hidden_state + mixture).astype(jnp.bfloat16)


def solution(mesh):
    in_specs = (
        P("sp", "tp"),
        P("sp", "tp"),
        P("sp", "tp"),
        P("tp"),
        P(None, "tp"),
        P(("sp", "tp"), None),
        P(),
        P(("sp", "tp"), None),
        P(("sp", "tp"), None),
        P("sp", None, "tp"),
        P("sp", None, "tp"),
        P("sp", "tp", None),
    )
    out_specs = P(("sp", "tp"), None)
    return jax.shard_map(local, mesh=mesh, in_specs=in_specs, out_specs=out_specs, check_vma=False)
```

```python
import functools

import jax
import jax.numpy as jnp
from jax import lax
from jax.experimental import pallas as pl
from jax.experimental.pallas import tpu as pltpu
from jax.sharding import PartitionSpec as P

HEADS = 32
KV_HEADS = 16
HEAD = 64
WINDOW = 128


EPS = 1e-06
NEGATIVE = -1e30
MESH = pl.DeviceIdType.MESH


def plane():
    t = lax.axis_index("tp")
    tx = t + 1 - 2 * lax.rem(t, 2)
    ty = lax.rem(t + 2, 4)
    return t, tx, ty, 3 - t


def greet(devices):
    barrier = pltpu.get_barrier_semaphore()
    for device in devices:
        pl.semaphore_signal(barrier, inc=1, device_id=device, device_id_type=MESH)
    pl.semaphore_wait(barrier, len(devices))


def remote(src, dst, send, recv, device):
    return pltpu.make_async_remote_copy(
        src_ref=src,
        dst_ref=dst,
        send_sem=send,
        recv_sem=recv,
        device_id=device,
        device_id_type=MESH,
    )


def dispatch_kernel(n, send_ref, out_ref, zs, zr, xs, xr, ys, yr, xhs, xhr, yhs, yhr):
    s = lax.axis_index("sp")
    t, tx, ty, _ = plane()
    half = send_ref.shape[1] // 2
    low, high = pl.ds(0, half), pl.ds(half, half)
    x_dev, y_dev = (s, tx), (s, ty)
    greet([(lax.rem(s + k, n), t) for k in range(1, n)] + [x_dev, y_dev])
    copies = []

    def go(*args):
        copy = remote(*args)
        copy.start()
        copies.append(copy)
        return copy

    incoming = [None]
    full = []

    def stage_a(j):
        source = lax.rem(s - j + n, n)
        if j:
            z_copies[j].wait_recv()
        src = out_ref.at[t, source] if j else send_ref.at[source]
        full.append(
            (
                go(src, out_ref.at[t, source], xs.at[j], xr.at[j], x_dev),
                go(src, out_ref.at[t, source], ys.at[j], yr.at[j], y_dev),
            )
        )

    halves = []

    def stage_b(j):
        source = lax.rem(s - j + n, n)
        full[j][0].wait_recv()
        part = out_ref.at[tx, source, low]
        halves.append(go(part, part, yhs.at[j], yhr.at[j], y_dev))
        full[j][1].wait_recv()
        part = out_ref.at[ty, source, high]
        halves.append(go(part, part, xhs.at[j], xhr.at[j], x_dev))

    z_copies = [None]
    for k in range(1, n):
        target = lax.rem(s + k, n)
        z_copies.append(
            go(send_ref.at[target], out_ref.at[t, s], zs.at[k], zr.at[k], (target, t))
        )
    stage_a(0)
    out_ref[t, s] = send_ref[s]
    for j in range(1, n):
        stage_a(j)
        stage_b(j - 1)
    stage_b(n - 1)
    for copy in halves:
        copy.wait_recv()
    for copy in copies:
        copy.wait_send()


def dispatch(sending):
    n, capacity, width = sending.shape
    sem = pltpu.SemaphoreType.DMA((n,))
    return pl.pallas_call(
        functools.partial(dispatch_kernel, n),
        out_shape=jax.ShapeDtypeStruct((4, n, capacity, width), sending.dtype),
        in_specs=[pl.BlockSpec(memory_space=pltpu.VMEM)],
        out_specs=pl.BlockSpec(memory_space=pltpu.VMEM),
        scratch_shapes=[sem] * 10,
        compiler_params=pltpu.CompilerParams(collective_id=0, has_side_effects=True),
    )(sending)


def return_kernel(
    n, part_ref, out_ref, bx1, by1, bx2, by2, acc, fin,
    x1s, x1r, y1s, y1r, x2s, x2r, y2s, y2r, zls, zlr, zhs, zhr,
):
    s = lax.axis_index("sp")
    t, tx, ty, td = plane()
    half = part_ref.shape[2] // 2
    low, high = pl.ds(0, half), pl.ds(half, half)
    x_dev, y_dev = (s, tx), (s, ty)
    greet([(lax.rem(s + k, n), t) for k in range(1, n)] + [x_dev, y_dev])
    copies = []

    def go(*args):
        copy = remote(*args)
        copy.start()
        copies.append(copy)
        return copy

    def total(a, b):
        return (a.astype(jnp.float32) + b.astype(jnp.float32)).astype(jnp.bfloat16)

    order = list(range(1, n)) + [0]
    first = []

    def begin(i):
        j = order[i]
        owner = lax.rem(s + j, n)
        first.append(
            (
                go(part_ref.at[td, owner, low], bx1.at[j, 1], x1s.at[j, 1], x1r.at[j, 1], x_dev),
                go(part_ref.at[td, owner, high], by1.at[j, 1], y1s.at[j, 1], y1r.at[j, 1], y_dev),
                go(part_ref.at[tx, owner, low], bx1.at[j, 0], x1s.at[j, 0], x1r.at[j, 0], x_dev),
                go(part_ref.at[ty, owner, high], by1.at[j, 0], y1s.at[j, 0], y1r.at[j, 0], y_dev),
            )
        )

    second = []
    back = []

    def middle(i):
        j = order[i]
        owner = lax.rem(s + j, n)
        first[i][0].wait_recv()
        acc[j, 0] = total(part_ref[ty, owner, low], bx1[j, 1])
        to_y = go(acc.at[j, 0], by2.at[j], y2s.at[j], y2r.at[j], y_dev)
        first[i][1].wait_recv()
        acc[j, 1] = total(part_ref[tx, owner, high], by1[j, 1])
        to_x = go(acc.at[j, 1], bx2.at[j], x2s.at[j], x2r.at[j], x_dev)
        second.append((to_y, to_x))

    def last(i):
        j = order[i]
        owner = lax.rem(s + j, n)
        first[i][2].wait_recv()
        second[i][0].wait_recv()
        lower = total(
            part_ref[t, owner, low].astype(jnp.float32) + bx1[j, 0].astype(jnp.float32), by2[j]
        )
        first[i][3].wait_recv()
        second[i][1].wait_recv()
        upper = total(
            part_ref[t, owner, high].astype(jnp.float32) + by1[j, 0].astype(jnp.float32), bx2[j]
        )
        if j:
            fin[j, low] = lower
            back.append(go(fin.at[j, low], out_ref.at[s, low], zls.at[j], zlr.at[j], (owner, t)))
            fin[j, high] = upper
            back.append(go(fin.at[j, high], out_ref.at[s, high], zhs.at[j], zhr.at[j], (owner, t)))
        else:
            out_ref[s, low] = lower
            out_ref[s, high] = upper

    begin(0)
    begin(1)
    middle(0)
    for i in range(1, n):
        if i + 1 < n:
            begin(i + 1)
        middle(i)
        last(i - 1)
    last(n - 1)
    for copy in back:
        copy.wait_recv()
    for copy in copies:
        copy.wait_send()


def give_back(partial_value):
    _, n, capacity, width = partial_value.shape
    half = capacity // 2
    kind = partial_value.dtype
    one = pltpu.SemaphoreType.DMA((n,))
    two = pltpu.SemaphoreType.DMA((n, 2))
    return pl.pallas_call(
        functools.partial(return_kernel, n),
        out_shape=jax.ShapeDtypeStruct((n, capacity, width), kind),
        in_specs=[pl.BlockSpec(memory_space=pltpu.VMEM)],
        out_specs=pl.BlockSpec(memory_space=pltpu.VMEM),
        scratch_shapes=[
            pltpu.VMEM((n, 2, half, width), kind),
            pltpu.VMEM((n, 2, half, width), kind),
            pltpu.VMEM((n, half, width), kind),
            pltpu.VMEM((n, half, width), kind),
            pltpu.VMEM((n, 2, half, width), kind),
            pltpu.VMEM((n, capacity, width), kind),
            two, two, two, two, one, one, one, one, one, one, one, one,
        ],
        compiler_params=pltpu.CompilerParams(collective_id=1, has_side_effects=True),
    )(partial_value)


def project_kernel(x_ref, w_ref, out_ref, buf, acc, cols, gs, gr, as_, ar):
    s = lax.axis_index("sp")
    t, tx, ty, td = plane()
    rows, depth = x_ref.shape
    half = rows // 2
    low, high = pl.ds(0, half), pl.ds(half, half)
    x_dev, y_dev, d_dev = (s, tx), (s, ty), (s, td)
    greet([x_dev, y_dev, d_dev])
    copies = []

    def go(*args):
        copy = remote(*args)
        copy.start()
        copies.append(copy)
        return copy

    def product(piece, owner, columns):
        weight = w_ref[pl.ds(pl.multiple_of(owner * depth, depth), depth), columns]
        return jnp.dot(piece, weight, preferred_element_type=jnp.float32)

    x_low = go(x_ref.at[low], buf.at[t, low], gs.at[0], gr.at[0], x_dev)
    y_high = go(x_ref.at[high], buf.at[t, high], gs.at[1], gr.at[1], y_dev)
    x_high = go(x_ref.at[high], buf.at[t, high], gs.at[2], gr.at[2], x_dev)
    y_low = go(x_ref.at[low], buf.at[t, low], gs.at[3], gr.at[3], y_dev)
    acc[...] = product(x_ref[...], t, slice(None))
    x_low.wait_recv()
    d_low = go(buf.at[tx, low], buf.at[tx, low], gs.at[4], gr.at[4], y_dev)
    y_high.wait_recv()
    d_high = go(buf.at[ty, high], buf.at[ty, high], gs.at[5], gr.at[5], x_dev)
    x_high.wait_recv()
    acc[...] += product(buf[tx], tx, slice(None))
    y_low.wait_recv()
    acc[...] += product(buf[ty], ty, slice(None))
    d_low.wait_recv()
    d_high.wait_recv()
    tiles = 2
    width = w_ref.shape[1] // tiles
    own = rows // 4
    arrivals = []
    for tile in range(tiles):
        columns = slice(tile * width, (tile + 1) * width)
        total = acc[:, columns] + product(buf[td], td, columns)
        cols[tile] = total.astype(cols.dtype)
        for k, (owner, device) in enumerate(((td, d_dev), (tx, x_dev), (ty, y_dev))):
            arrivals.append(
                go(
                    cols.at[tile, pl.ds(pl.multiple_of(owner * own, own), own)],
                    out_ref.at[tile, t],
                    as_.at[tile, k],
                    ar.at[tile, k],
                    device,
                )
            )
        out_ref[tile, t] = cols[tile, pl.ds(pl.multiple_of(t * own, own), own)]
    for copy in arrivals:
        copy.wait_recv()
    for copy in copies:
        copy.wait_send()


def project(attention, out_weight):
    rows, depth = attention.shape
    width = out_weight.shape[1]
    kind = attention.dtype
    out = pl.pallas_call(
        project_kernel,
        out_shape=jax.ShapeDtypeStruct((2, 4, rows // 4, width // 2), kind),
        in_specs=[pl.BlockSpec(memory_space=pltpu.VMEM)] * 2,
        out_specs=pl.BlockSpec(memory_space=pltpu.VMEM),
        scratch_shapes=[
            pltpu.VMEM((4, rows, depth), kind),
            pltpu.VMEM((rows, width), jnp.float32),
            pltpu.VMEM((2, rows, width // 2), kind),
            pltpu.SemaphoreType.DMA((6,)),
            pltpu.SemaphoreType.DMA((6,)),
            pltpu.SemaphoreType.DMA((2, 3)),
            pltpu.SemaphoreType.DMA((2, 3)),
        ],
        compiler_params=pltpu.CompilerParams(collective_id=2, has_side_effects=True),
    )(attention, out_weight)
    return out.transpose(2, 1, 0, 3).reshape(rows // 4, 4 * width)


def with_halo(block, sides, width):
    for axis, dim in sides:
        count = lax.axis_size(axis)
        forward = [(i, i + 1) for i in range(count - 1)]
        backward = [(target, source) for source, target in forward]
        low = lax.ppermute(
            lax.slice_in_dim(block, block.shape[dim] - width, None, axis=dim), axis, forward
        )
        high = lax.ppermute(lax.slice_in_dim(block, 0, width, axis=dim), axis, backward)
        block = jnp.concatenate([low, block, high], axis=dim)
    return block


def make_band(extended, length):
    blocks = length // WINDOW
    pieces = [
        lax.slice_in_dim(extended, offset * WINDOW, offset * WINDOW + length, axis=0).reshape(
            blocks, WINDOW, -1
        )
        for offset in range(3)
    ]
    return jnp.concatenate(pieces, axis=1)


def attend_local(queries, keys, values, sink_logit):
    length = queries.shape[0]
    groups = keys.shape[1] // HEAD
    repeat = HEADS // KV_HEADS
    blocks = length // WINDOW
    joined = jnp.concatenate([keys, values], axis=1)
    extended = with_halo(joined, (("sp", 0),), WINDOW)
    banded = make_band(extended, length)
    key_band = banded[..., : groups * HEAD].reshape(blocks, 3 * WINDOW, groups, HEAD)
    value_band = banded[..., groups * HEAD :].reshape(blocks, 3 * WINDOW, groups, HEAD)
    query_blocks = queries.reshape(blocks, WINDOW, groups, repeat, HEAD)
    scores = jnp.einsum(
        "nqgrd,nkgd->ngrqk", query_blocks, key_band, preferred_element_type=jnp.float32
    ) * HEAD ** (-0.5)
    near = jnp.abs(jnp.arange(WINDOW)[:, None] + WINDOW - jnp.arange(3 * WINDOW)[None, :]) <= WINDOW
    first_token = lax.axis_index("sp") * length
    key_pos = (
        first_token + (jnp.arange(blocks)[:, None] - 1) * WINDOW + jnp.arange(3 * WINDOW)[None, :]
    )
    inside = (key_pos >= 0) & (key_pos < length * lax.axis_size("sp"))
    valid = near[None, None, None, :, :] & inside[:, None, None, None, :]
    sinks = sink_logit.reshape(1, groups, repeat, 1, 1)
    masked = jnp.where(valid, scores, NEGATIVE)
    top = jnp.maximum(jnp.max(masked, axis=-1, keepdims=True), sinks)
    probs = jnp.exp(masked - top)
    denom = jnp.sum(probs, axis=-1, keepdims=True) + jnp.exp(sinks - top)
    weights = (probs / denom).astype(jnp.bfloat16)
    output = jnp.einsum(
        "ngrqk,nkgd->nqgrd", weights, value_band, preferred_element_type=jnp.float32
    )
    return output.astype(jnp.bfloat16).reshape(length, groups * repeat * HEAD)


def local(
    queries,
    keys,
    values,
    sink_logit,
    out_weight,
    residual,
    norm_gain,
    routes,
    route_weights,
    gate_weight,
    up_weight,
    down_weight,
):
    attention = attend_local(queries, keys, values, sink_logit)
    capacity = max(2, 4 * residual.shape[0] // lax.axis_size("sp"))
    in_plane = lax.axis_size("tp") == 4 and capacity % 32 == 0
    if in_plane:
        projected = project(attention, out_weight)
    else:
        columns = jnp.dot(
            lax.all_gather(attention, "tp", axis=1, tiled=True),
            out_weight,
            preferred_element_type=jnp.float32,
        )
        projected = lax.all_to_all(
            columns.astype(jnp.bfloat16), "tp", split_axis=0, concat_axis=1, tiled=True
        )
    hidden_state = residual.astype(jnp.float32) + projected.astype(jnp.float32)
    inverse = lax.rsqrt(jnp.mean(hidden_state * hidden_state, axis=-1, keepdims=True) + EPS)
    normed = (hidden_state * inverse * norm_gain).astype(jnp.bfloat16)
    sp_count = lax.axis_size("sp")
    tok_rows = residual.shape[0]
    width = residual.shape[1]
    slot_total = sp_count * capacity
    expert_ids = routes.reshape(-1)
    onehot = (expert_ids[:, None] == jnp.arange(sp_count, dtype=jnp.int32)[None, :]).astype(
        jnp.int32
    )
    earlier = jnp.cumsum(onehot, axis=0) - onehot
    rank = jnp.sum(earlier * onehot, axis=1)
    slots = expert_ids * capacity + rank
    placing = (slots[:, None] == jnp.arange(slot_total, dtype=jnp.int32)[None, :]).astype(
        jnp.bfloat16
    )
    placing = placing.reshape(tok_rows, 2, slot_total)
    first_place = placing[:, 0]
    second_place = placing[:, 1]
    sending = jnp.einsum(
        "ts,td->sd", first_place + second_place, normed, preferred_element_type=jnp.float32
    )
    sending = sending.astype(jnp.bfloat16).reshape(sp_count, capacity, width)
    if in_plane:
        piece = dispatch(sending)
    else:
        piece = lax.all_gather(
            lax.all_to_all(sending, "sp", split_axis=0, concat_axis=0, tiled=True),
            "tp",
            axis=0,
            tiled=True,
        )
    flat = piece.reshape(-1, piece.shape[-1])
    gate = jnp.dot(flat, gate_weight[0], preferred_element_type=jnp.float32)
    upward = jnp.dot(flat, up_weight[0], preferred_element_type=jnp.float32)
    hidden = (jax.nn.silu(gate) * upward).astype(jnp.bfloat16)
    partial_value = jnp.dot(hidden, down_weight[0], preferred_element_type=jnp.float32)
    partial_value = partial_value.reshape(piece.shape[:-1] + (down_weight.shape[-1],))
    partial_value = partial_value.astype(jnp.bfloat16)
    if in_plane:
        returned = give_back(partial_value)
    else:
        returned = lax.all_to_all(
            lax.psum_scatter(partial_value, "tp", scatter_dimension=0, tiled=True),
            "sp",
            split_axis=0,
            concat_axis=0,
            tiled=True,
        )
    gathered_back = returned.reshape(slot_total, width)
    first_pick = jnp.dot(first_place, gathered_back, preferred_element_type=jnp.float32)
    second_pick = jnp.dot(second_place, gathered_back, preferred_element_type=jnp.float32)
    mixture = route_weights[:, 0:1] * first_pick + route_weights[:, 1:2] * second_pick
    return (hidden_state + mixture).astype(jnp.bfloat16)


def solution(mesh):
    in_specs = (
        P("sp", "tp"),
        P("sp", "tp"),
        P("sp", "tp"),
        P("tp"),
        P(None, "tp"),
        P(("sp", "tp"), None),
        P(),
        P(("sp", "tp"), None),
        P(("sp", "tp"), None),
        P("sp", None, "tp"),
        P("sp", None, "tp"),
        P("sp", "tp", None),
    )
    out_specs = P(("sp", "tp"), None)
    return jax.shard_map(local, mesh=mesh, in_specs=in_specs, out_specs=out_specs, check_vma=False)
```

```python
import functools

import jax
import jax.numpy as jnp
from jax import lax
from jax.experimental import pallas as pl
from jax.experimental.pallas import tpu as pltpu
from jax.sharding import PartitionSpec as P

HEADS = 32
KV_HEADS = 16
HEAD = 64
WINDOW = 128


EPS = 1e-06
NEGATIVE = -1e30
MESH = pl.DeviceIdType.MESH


def plane():
    t = lax.axis_index("tp")
    tx = t + 1 - 2 * lax.rem(t, 2)
    ty = lax.rem(t + 2, 4)
    return t, tx, ty, 3 - t


def greet(devices):
    barrier = pltpu.get_barrier_semaphore()
    for device in devices:
        pl.semaphore_signal(barrier, inc=1, device_id=device, device_id_type=MESH)
    pl.semaphore_wait(barrier, len(devices))


def remote(src, dst, send, recv, device):
    return pltpu.make_async_remote_copy(
        src_ref=src,
        dst_ref=dst,
        send_sem=send,
        recv_sem=recv,
        device_id=device,
        device_id_type=MESH,
    )


def flipped(index, mask):
    result = index
    bit = 1
    while bit <= mask:
        if mask & bit:
            result = result + bit * (1 - 2 * lax.rem(index // bit, 2))
        bit *= 2
    return result


def expert_kernel(
    send_ref, gate_hbm, up_hbm, down_hbm, out_ref,
    gate, up, down, piece, hidden, part, bx1, by1, bx2, by2, acc, fin, load,
    zs, zr, xs, xr, ys, yr, xhs, xhr, yhs, yhr,
    x1s, x1r, y1s, y1r, x2s, x2r, y2s, y2r, zls, zlr, zhs, zhr,
):
    n, capacity, width = send_ref.shape
    s = lax.axis_index("sp")
    t, tx, ty, td = plane()
    half = capacity // 2
    low, high = pl.ds(0, half), pl.ds(half, half)
    x_dev, y_dev = (s, tx), (s, ty)
    loads = [
        pltpu.make_async_copy(source, target, load.at[k])
        for k, (source, target) in enumerate(((gate_hbm, gate), (up_hbm, up), (down_hbm, down)))
    ]
    for copy in loads:
        copy.start()
    greet([(flipped(s, m), t) for m in range(1, n)] + [x_dev, y_dev])
    copies = []

    def go(*args):
        copy = remote(*args)
        copy.start()
        copies.append(copy)
        return copy

    def total(a, b):
        return (a.astype(jnp.float32) + b.astype(jnp.float32)).astype(jnp.bfloat16)

    gray = [k ^ (k >> 1) for k in range(n // 2)]
    z_copies, full, halves, first, second, back = {}, {}, {}, {}, {}, []

    def members(q):
        return (2 * q, 2 * q + 1)

    def stage_a(q):
        for m in members(q):
            source = flipped(s, m)
            if m:
                z_copies[m].wait_recv()
            src = piece.at[t, source] if m else send_ref.at[source]
            full[m] = (
                go(src, piece.at[t, source], xs.at[m], xr.at[m], x_dev),
                go(src, piece.at[t, source], ys.at[m], yr.at[m], y_dev),
            )

    def stage_b(q):
        for m in members(q):
            source = flipped(s, m)
            full[m][0].wait_recv()
            block = piece.at[tx, source, low]
            to_y = go(block, block, yhs.at[m], yhr.at[m], y_dev)
            full[m][1].wait_recv()
            block = piece.at[ty, source, high]
            halves[m] = (to_y, go(block, block, xhs.at[m], xhr.at[m], x_dev))

    def compute(q):
        for m in members(q):
            for copy in halves[m]:
                copy.wait_recv()
        base = flipped(s // 2, q) * 2
        rows = 8 * capacity
        step = 256

        @pl.loop(0, gate.shape[1] // step)
        def _(k):
            columns = pl.ds(pl.multiple_of(k * step, step), step)
            x = piece[:, pl.ds(base, 2)].reshape(rows, width)
            g = jnp.dot(x, gate[:, columns], preferred_element_type=jnp.float32)
            u = jnp.dot(x, up[:, columns], preferred_element_type=jnp.float32)
            hidden[:, columns] = (jax.nn.silu(g) * u).astype(hidden.dtype)

        wide = 512

        @pl.loop(0, width // wide)
        def _(k):
            columns = pl.ds(pl.multiple_of(k * wide, wide), wide)
            share = jnp.dot(hidden[...], down[:, columns], preferred_element_type=jnp.float32)
            part[:, pl.ds(base, 2), :, columns] = share.astype(part.dtype).reshape(
                4, 2, capacity, wide
            )

    def begin(q):
        for m in members(q):
            owner = flipped(s, m)
            first[m] = (
                go(part.at[td, owner, low], bx1.at[m, 1], x1s.at[m, 1], x1r.at[m, 1], x_dev),
                go(part.at[td, owner, high], by1.at[m, 1], y1s.at[m, 1], y1r.at[m, 1], y_dev),
                go(part.at[tx, owner, low], bx1.at[m, 0], x1s.at[m, 0], x1r.at[m, 0], x_dev),
                go(part.at[ty, owner, high], by1.at[m, 0], y1s.at[m, 0], y1r.at[m, 0], y_dev),
            )

    def middle(q):
        for m in members(q):
            owner = flipped(s, m)
            first[m][0].wait_recv()
            acc[m, 0] = total(part[ty, owner, low], bx1[m, 1])
            to_y = go(acc.at[m, 0], by2.at[m], y2s.at[m], y2r.at[m], y_dev)
            first[m][1].wait_recv()
            acc[m, 1] = total(part[tx, owner, high], by1[m, 1])
            second[m] = (to_y, go(acc.at[m, 1], bx2.at[m], x2s.at[m], x2r.at[m], x_dev))

    def last(q):
        for m in members(q):
            owner = flipped(s, m)
            first[m][2].wait_recv()
            second[m][0].wait_recv()
            lower = total(
                part[t, owner, low].astype(jnp.float32) + bx1[m, 0].astype(jnp.float32), by2[m]
            )
            first[m][3].wait_recv()
            second[m][1].wait_recv()
            upper = total(
                part[t, owner, high].astype(jnp.float32) + by1[m, 0].astype(jnp.float32), bx2[m]
            )
            if m:
                away = (owner, t)
                fin[m, low] = lower
                back.append(go(fin.at[m, low], out_ref.at[s, low], zls.at[m], zlr.at[m], away))
                fin[m, high] = upper
                back.append(go(fin.at[m, high], out_ref.at[s, high], zhs.at[m], zhr.at[m], away))
            else:
                out_ref[s, low] = lower
                out_ref[s, high] = upper

    for q in gray:
        for m in members(q):
            if m:
                target = flipped(s, m)
                z_copies[m] = go(
                    send_ref.at[target], piece.at[t, s], zs.at[m], zr.at[m], (target, t)
                )
    stage_a(0)
    piece[t, s] = send_ref[s]
    order = gray[1:] + [0]
    count = len(gray)
    for k in range(count + 4):
        if k + 1 < count:
            stage_a(gray[k + 1])
        if k < count:
            stage_b(gray[k])
        if k == 2:
            for copy in loads:
                copy.wait()
        if 0 <= k - 2 < count:
            compute(order[k - 2])
            begin(order[k - 2])
        if 0 <= k - 3 < count:
            middle(order[k - 3])
        if 0 <= k - 4 < count:
            last(order[k - 4])
    for copy in back:
        copy.wait_recv()
    for copy in copies:
        copy.wait_send()


def experts(sending, gate_weight, up_weight, down_weight):
    n, capacity, width = sending.shape
    half = capacity // 2
    kind = sending.dtype
    one = pltpu.SemaphoreType.DMA((n,))
    two = pltpu.SemaphoreType.DMA((n, 2))
    anywhere = pl.BlockSpec(memory_space=pl.ANY)
    return pl.pallas_call(
        expert_kernel,
        out_shape=jax.ShapeDtypeStruct((n, capacity, width), kind),
        in_specs=[pl.BlockSpec(memory_space=pltpu.VMEM), anywhere, anywhere, anywhere],
        out_specs=pl.BlockSpec(memory_space=pltpu.VMEM),
        scratch_shapes=[
            pltpu.VMEM(gate_weight.shape, kind),
            pltpu.VMEM(up_weight.shape, kind),
            pltpu.VMEM(down_weight.shape, kind),
            pltpu.VMEM((4, n, capacity, width), kind),
            pltpu.VMEM((8 * capacity, gate_weight.shape[1]), kind),
            pltpu.VMEM((4, n, capacity, width), kind),
            pltpu.VMEM((n, 2, half, width), kind),
            pltpu.VMEM((n, 2, half, width), kind),
            pltpu.VMEM((n, half, width), kind),
            pltpu.VMEM((n, half, width), kind),
            pltpu.VMEM((n, 2, half, width), kind),
            pltpu.VMEM((n, capacity, width), kind),
            pltpu.SemaphoreType.DMA((3,)),
        ]
        + [one] * 10
        + [two] * 4
        + [one] * 8,
        compiler_params=pltpu.CompilerParams(
            collective_id=0, has_side_effects=True, vmem_limit_bytes=56 * 1024 * 1024
        ),
    )(sending, gate_weight, up_weight, down_weight)


def project_kernel(x_ref, w_ref, out_ref, buf, acc, cols, gs, gr, as_, ar):
    s = lax.axis_index("sp")
    t, tx, ty, td = plane()
    rows, depth = x_ref.shape
    half = rows // 2
    low, high = pl.ds(0, half), pl.ds(half, half)
    x_dev, y_dev, d_dev = (s, tx), (s, ty), (s, td)
    greet([x_dev, y_dev, d_dev])
    copies = []

    def go(*args):
        copy = remote(*args)
        copy.start()
        copies.append(copy)
        return copy

    def product(piece, owner, columns):
        weight = w_ref[pl.ds(pl.multiple_of(owner * depth, depth), depth), columns]
        return jnp.dot(piece, weight, preferred_element_type=jnp.float32)

    x_low = go(x_ref.at[low], buf.at[t, low], gs.at[0], gr.at[0], x_dev)
    y_high = go(x_ref.at[high], buf.at[t, high], gs.at[1], gr.at[1], y_dev)
    x_high = go(x_ref.at[high], buf.at[t, high], gs.at[2], gr.at[2], x_dev)
    y_low = go(x_ref.at[low], buf.at[t, low], gs.at[3], gr.at[3], y_dev)
    acc[...] = product(x_ref[...], t, slice(None))
    x_low.wait_recv()
    d_low = go(buf.at[tx, low], buf.at[tx, low], gs.at[4], gr.at[4], y_dev)
    y_high.wait_recv()
    d_high = go(buf.at[ty, high], buf.at[ty, high], gs.at[5], gr.at[5], x_dev)
    x_high.wait_recv()
    acc[...] += product(buf[tx], tx, slice(None))
    y_low.wait_recv()
    acc[...] += product(buf[ty], ty, slice(None))
    d_low.wait_recv()
    d_high.wait_recv()
    tiles = 2
    width = w_ref.shape[1] // tiles
    own = rows // 4
    arrivals = []
    for tile in range(tiles):
        columns = slice(tile * width, (tile + 1) * width)
        total = acc[:, columns] + product(buf[td], td, columns)
        cols[tile] = total.astype(cols.dtype)
        for k, (owner, device) in enumerate(((td, d_dev), (tx, x_dev), (ty, y_dev))):
            arrivals.append(
                go(
                    cols.at[tile, pl.ds(pl.multiple_of(owner * own, own), own)],
                    out_ref.at[tile, t],
                    as_.at[tile, k],
                    ar.at[tile, k],
                    device,
                )
            )
        out_ref[tile, t] = cols[tile, pl.ds(pl.multiple_of(t * own, own), own)]
    for copy in arrivals:
        copy.wait_recv()
    for copy in copies:
        copy.wait_send()


def project(attention, out_weight):
    rows, depth = attention.shape
    width = out_weight.shape[1]
    kind = attention.dtype
    out = pl.pallas_call(
        project_kernel,
        out_shape=jax.ShapeDtypeStruct((2, 4, rows // 4, width // 2), kind),
        in_specs=[pl.BlockSpec(memory_space=pltpu.VMEM)] * 2,
        out_specs=pl.BlockSpec(memory_space=pltpu.VMEM),
        scratch_shapes=[
            pltpu.VMEM((4, rows, depth), kind),
            pltpu.VMEM((rows, width), jnp.float32),
            pltpu.VMEM((2, rows, width // 2), kind),
            pltpu.SemaphoreType.DMA((6,)),
            pltpu.SemaphoreType.DMA((6,)),
            pltpu.SemaphoreType.DMA((2, 3)),
            pltpu.SemaphoreType.DMA((2, 3)),
        ],
        compiler_params=pltpu.CompilerParams(collective_id=2, has_side_effects=True),
    )(attention, out_weight)
    return out.transpose(2, 1, 0, 3).reshape(rows // 4, 4 * width)


def with_halo(block, sides, width):
    for axis, dim in sides:
        count = lax.axis_size(axis)
        forward = [(i, i + 1) for i in range(count - 1)]
        backward = [(target, source) for source, target in forward]
        low = lax.ppermute(
            lax.slice_in_dim(block, block.shape[dim] - width, None, axis=dim), axis, forward
        )
        high = lax.ppermute(lax.slice_in_dim(block, 0, width, axis=dim), axis, backward)
        block = jnp.concatenate([low, block, high], axis=dim)
    return block


def make_band(extended, length):
    blocks = length // WINDOW
    pieces = [
        lax.slice_in_dim(extended, offset * WINDOW, offset * WINDOW + length, axis=0).reshape(
            blocks, WINDOW, -1
        )
        for offset in range(3)
    ]
    return jnp.concatenate(pieces, axis=1)


def attend_local(queries, keys, values, sink_logit):
    length = queries.shape[0]
    groups = keys.shape[1] // HEAD
    repeat = HEADS // KV_HEADS
    blocks = length // WINDOW
    joined = jnp.concatenate([keys, values], axis=1)
    extended = with_halo(joined, (("sp", 0),), WINDOW)
    banded = make_band(extended, length)
    key_band = banded[..., : groups * HEAD].reshape(blocks, 3 * WINDOW, groups, HEAD)
    value_band = banded[..., groups * HEAD :].reshape(blocks, 3 * WINDOW, groups, HEAD)
    query_blocks = queries.reshape(blocks, WINDOW, groups, repeat, HEAD)
    scores = jnp.einsum(
        "nqgrd,nkgd->ngrqk", query_blocks, key_band, preferred_element_type=jnp.float32
    ) * HEAD ** (-0.5)
    near = jnp.abs(jnp.arange(WINDOW)[:, None] + WINDOW - jnp.arange(3 * WINDOW)[None, :]) <= WINDOW
    first_token = lax.axis_index("sp") * length
    key_pos = (
        first_token + (jnp.arange(blocks)[:, None] - 1) * WINDOW + jnp.arange(3 * WINDOW)[None, :]
    )
    inside = (key_pos >= 0) & (key_pos < length * lax.axis_size("sp"))
    valid = near[None, None, None, :, :] & inside[:, None, None, None, :]
    sinks = sink_logit.reshape(1, groups, repeat, 1, 1)
    masked = jnp.where(valid, scores, NEGATIVE)
    top = jnp.maximum(jnp.max(masked, axis=-1, keepdims=True), sinks)
    probs = jnp.exp(masked - top)
    denom = jnp.sum(probs, axis=-1, keepdims=True) + jnp.exp(sinks - top)
    weights = (probs / denom).astype(jnp.bfloat16)
    output = jnp.einsum(
        "ngrqk,nkgd->nqgrd", weights, value_band, preferred_element_type=jnp.float32
    )
    return output.astype(jnp.bfloat16).reshape(length, groups * repeat * HEAD)


def local(
    queries,
    keys,
    values,
    sink_logit,
    out_weight,
    residual,
    norm_gain,
    routes,
    route_weights,
    gate_weight,
    up_weight,
    down_weight,
):
    attention = attend_local(queries, keys, values, sink_logit)
    capacity = max(2, 4 * residual.shape[0] // lax.axis_size("sp"))
    in_plane = (
        lax.axis_size("tp") == 4
        and lax.axis_size("sp") == 8
        and capacity % 32 == 0
        and gate_weight.shape[2] % 256 == 0
    )
    if in_plane:
        projected = project(attention, out_weight)
    else:
        columns = jnp.dot(
            lax.all_gather(attention, "tp", axis=1, tiled=True),
            out_weight,
            preferred_element_type=jnp.float32,
        )
        projected = lax.all_to_all(
            columns.astype(jnp.bfloat16), "tp", split_axis=0, concat_axis=1, tiled=True
        )
    hidden_state = residual.astype(jnp.float32) + projected.astype(jnp.float32)
    inverse = lax.rsqrt(jnp.mean(hidden_state * hidden_state, axis=-1, keepdims=True) + EPS)
    normed = (hidden_state * inverse * norm_gain).astype(jnp.bfloat16)
    sp_count = lax.axis_size("sp")
    tok_rows = residual.shape[0]
    width = residual.shape[1]
    slot_total = sp_count * capacity
    expert_ids = routes.reshape(-1)
    onehot = (expert_ids[:, None] == jnp.arange(sp_count, dtype=jnp.int32)[None, :]).astype(
        jnp.int32
    )
    earlier = jnp.cumsum(onehot, axis=0) - onehot
    rank = jnp.sum(earlier * onehot, axis=1)
    slots = expert_ids * capacity + rank
    placing = (slots[:, None] == jnp.arange(slot_total, dtype=jnp.int32)[None, :]).astype(
        jnp.bfloat16
    )
    placing = placing.reshape(tok_rows, 2, slot_total)
    first_place = placing[:, 0]
    second_place = placing[:, 1]
    sending = jnp.einsum(
        "ts,td->sd", first_place + second_place, normed, preferred_element_type=jnp.float32
    )
    sending = sending.astype(jnp.bfloat16).reshape(sp_count, capacity, width)
    if in_plane:
        returned = experts(sending, gate_weight[0], up_weight[0], down_weight[0])
    else:
        piece = lax.all_gather(
            lax.all_to_all(sending, "sp", split_axis=0, concat_axis=0, tiled=True),
            "tp",
            axis=0,
            tiled=True,
        )
        flat = piece.reshape(-1, piece.shape[-1])
        gate = jnp.dot(flat, gate_weight[0], preferred_element_type=jnp.float32)
        upward = jnp.dot(flat, up_weight[0], preferred_element_type=jnp.float32)
        hidden = (jax.nn.silu(gate) * upward).astype(jnp.bfloat16)
        partial_value = jnp.dot(hidden, down_weight[0], preferred_element_type=jnp.float32)
        partial_value = partial_value.reshape(piece.shape[:-1] + (down_weight.shape[-1],))
        returned = lax.all_to_all(
            lax.psum_scatter(
                partial_value.astype(jnp.bfloat16), "tp", scatter_dimension=0, tiled=True
            ),
            "sp",
            split_axis=0,
            concat_axis=0,
            tiled=True,
        )
    gathered_back = returned.reshape(slot_total, width)
    first_pick = jnp.dot(first_place, gathered_back, preferred_element_type=jnp.float32)
    second_pick = jnp.dot(second_place, gathered_back, preferred_element_type=jnp.float32)
    mixture = route_weights[:, 0:1] * first_pick + route_weights[:, 1:2] * second_pick
    return (hidden_state + mixture).astype(jnp.bfloat16)


def solution(mesh):
    in_specs = (
        P("sp", "tp"),
        P("sp", "tp"),
        P("sp", "tp"),
        P("tp"),
        P(None, "tp"),
        P(("sp", "tp"), None),
        P(),
        P(("sp", "tp"), None),
        P(("sp", "tp"), None),
        P("sp", None, "tp"),
        P("sp", None, "tp"),
        P("sp", "tp", None),
    )
    out_specs = P(("sp", "tp"), None)
    return jax.shard_map(local, mesh=mesh, in_specs=in_specs, out_specs=out_specs, check_vma=False)
```
